128 devices in a mesh: sp: 64 (over z, y, x), tp: 2 (over core).
Axes of the slice: x: 4, y: 4, z: 4, core: 2. Of those that a mesh axis runs over, the one named last changes fastest.
Arguments:
- pool_input: bfloat16 [32768, 512], P('sp', 'tp'), may hold values from -8 to 8
- documents: int32 [32768], P('sp'), may hold values from 0 to 15, never falling along the last dimension, each value on 1 to 4096 neighbouring positions
- residual: bfloat16 [32768, 2048], P(('sp', 'tp')), may hold values from -6 to 6
- group_weights: bfloat16 [8, 64, 64], replicated, may hold values from -0.75 to 0.75
- pool_gain: bfloat16 [512], replicated, may hold values from 0.099609375 to 1.8984375
- output_weight: bfloat16 [512, 2048], replicated, may hold values from -0.25 to 0.25
- mixer_gain: bfloat16 [2048], replicated, may hold values from 0.099609375 to 1.8984375
- routed_gain: bfloat16 [2048], replicated, may hold values from 0.099609375 to 1.8984375
- final_gain: bfloat16 [2048], replicated, may hold values from 0.099609375 to 1.8984375
- chosen_group: int32 [32768, 1], P(('sp', 'tp')), may hold values from 0 to 63; in each aligned block of 256 rows (0 to 255, 256 to 511, ...) at most 8 rows name the same one
- chosen_experts: int32 [32768, 2], P(('sp', 'tp')), may hold values from 0 to 2, all different within a row
- expert_share: bfloat16 [32768, 2], P(('sp', 'tp')), may hold values from 0.099609375 to 1
- expert_gate: bfloat16 [192, 2048, 1024], P('sp', None, 'tp'), may hold values from -0.125 to 0.125
- expert_up: bfloat16 [192, 2048, 1024], P('sp', None, 'tp'), may hold values from -0.125 to 0.125
- expert_down: bfloat16 [192, 1024, 2048], P('sp', 'tp'), may hold values from -0.1875 to 0.1875
Outputs:
- updated: bfloat16 [32768, 2048], P(('sp', 'tp'))
The draws below stay inside these ranges and needn't reach their ends.
Inputs may be any that keep to these rules, and one draw needn't show every extreme that they name: `documents`: document numbers never fall along the sequence; every number appears, and a document holds 1 to 4096 positions. `chosen_group`: among the rows of one device at most 8 name the same group, and in every draw some group is named by exactly 8 rows of some device. `chosen_experts`: each row names 2 different experts of its group.
All inputs are finite; a program needn't handle non-finite values.
Results may differ from the reference program's by a relative error of at most 0.012.
Values may be sent and summed in bfloat16 or wider, within the bound.
No kernel may reach another device: no remote copies, remote signals or barrier semaphores. Data moves between devices by JAX's collectives and lax.ppermute only.
A program may use at most 128 MiB of HBM per device.

```python
import math
import jax
import jax.numpy as jnp
import numpy as np
from jax import lax

D = 2048
POOL_GROUPS = 8
GROUP_DIM = 64
POOL_WIDTH = 512
FFE = 1024
EPG = 3
TOPK = 2
TOK_DEV = 512
TOKENS = 32768
ROWS = 256
HALO = 256
WIN_S = 128
WIN_M = 256
WIN_L = 512
DOCS = 16
DOC_MAX = 4096
GROUPS = 64
EXPERTS = 192
CAP = 8
FFE_PART = 512
N_TP = 2


def draw_pool_input(key, part):
    noise_key = jax.random.fold_in(key, 11)
    coarse_key = jax.random.fold_in(key, 12)
    fine_key = jax.random.fold_in(key, 13)
    coarse = jax.random.normal(coarse_key, (TOKENS // HALO, POOL_WIDTH), jnp.float32)
    fine = jax.random.normal(fine_key, (TOKENS // (TOK_DEV // 8), POOL_WIDTH), jnp.float32)
    offsets = jnp.repeat(coarse, HALO, axis=0) + 0.7 * jnp.repeat(fine, TOK_DEV // 8, axis=0)
    values = jax.random.normal(noise_key, (TOKENS, POOL_WIDTH), jnp.float32) + offsets
    return jnp.clip(values, -8.0, 8.0).astype(jnp.bfloat16)


def block_scale(key, shape, cuts, low, largest):
    level, own = 1.0, jax.random.fold_in(key, 6)
    for position, parts in cuts:
        draws = jnp.exp(jax.random.uniform(jax.random.fold_in(own, position), (parts,), jnp.float32, low / len(cuts), largest / len(cuts)))
        level = level * jnp.repeat(draws, shape[position] // parts).reshape([-1 if axis == position else 1 for axis in range(len(shape))])
    return level


def choose_distinct(rng, rows, number_of, top, lift):
    ranking = jax.random.permutation(jax.random.fold_in(rng, 1), number_of)
    favour = ranking
    for power in range(3):
        favour = favour * favour // number_of
    favour = favour * lift // number_of
    lots = jax.random.randint(jax.random.fold_in(rng, 2), (rows, number_of), 0, 4096) + favour
    fixed_rows = jax.random.permutation(jax.random.fold_in(rng, 3), rows)[jnp.arange(number_of) % rows]
    lots = jnp.where(jnp.arange(rows)[:, None] == fixed_rows[None, :], 1 << 14, lots)
    merit = lots * number_of + jnp.arange(number_of)
    return lax.top_k(merit.astype(jnp.int32), top)[1].astype(jnp.int32)


def profile(count, total, most, skew):
    portions = [(1 << 20) // math.isqrt(standing ** skew) + 1 for standing in range(2, count + 1)]
    spare, given = total - most - (count - 1), [1] * (count - 1)
    while spare > 0:
        free = [i for i in range(count - 1) if given[i] < most]
        pool, budget = sum([portions[i] for i in free]), spare
        for i in free:
            addition = min(most - given[i], max(1, budget * portions[i] // pool), spare)
            given[i] = given[i] + addition
            spare = spare - addition
    return np.array([most] + given)


def uneven(key, number_of, total, bound, skew):
    if number_of == 2:
        one = jax.random.randint(key, (), max(1, total - bound), min(bound, total - 1) + 1)
        return jnp.stack([one, total - one])
    sizes = jnp.asarray(profile(number_of, total, bound, skew), jnp.int32)
    twos = (number_of - 1) // 2
    donor, sink = sizes[1:1 + 2 * twos:2], sizes[2:2 + 2 * twos:2]
    margin = jnp.minimum(donor - 1, bound - sink)
    passed = jax.random.randint(jax.random.fold_in(key, 1), (twos,), 0, 1 << 20) % (margin + 1)
    sizes = sizes.at[1:1 + 2 * twos:2].set(donor - passed).at[2:2 + 2 * twos:2].set(sink + passed)
    return sizes[jax.random.permutation(jax.random.fold_in(key, 2), number_of)]


def routed_block(key, own, number, rows, count, top, limit, skew):
    ranking = jax.random.permutation(key, count)
    packed, common = portions_of(count, rows * top, limit, skew, True), portions_of(count, rows * top, limit, skew, False)
    places = jnp.arange(count)

    def named(tallies, offset_by):
        used = int((tallies > 0).sum())
        fixed = max(1, used // 4)
        passed = fixed + (places - fixed + offset_by * (used - fixed)) % max(1, count - fixed)
        return jnp.zeros((count,), jnp.int32).at[ranking[jnp.where(places < fixed, places, passed)]].set(jnp.asarray(tallies, jnp.int32))

    tallies = jnp.where(number % 4 == 0, named(packed, number // 4), named(common, number - number // 4 - 1))
    mixed = jax.random.permutation(jax.random.fold_in(own, 3), count)
    donor, sink = mixed[0:count // 2 * 2:2], mixed[1:count // 2 * 2:2]
    room = jnp.minimum(tallies[donor] - 1, limit - tallies[sink]) // 2
    room = jnp.where((donor == ranking[0]) | (sink == ranking[0]) | (tallies[sink] == 0), 0, jnp.maximum(room, 0))
    passed = jax.random.randint(jax.random.fold_in(own, 4), (count // 2,), 0, 1 << 20) % (room + 1)
    tallies = tallies.at[donor].add(-passed).at[sink].add(passed)
    items = jnp.searchsorted(jnp.cumsum(tallies), jnp.arange(rows * top), side="right").astype(jnp.int32)
    table = items.reshape(top, rows).T
    table = table[jax.random.permutation(jax.random.fold_in(own, 1), rows)]
    offset_by = jax.random.randint(jax.random.fold_in(own, 2), (rows, 1), 0, top)
    return jnp.take_along_axis(table, (jnp.arange(top)[None, :] + offset_by) % top, axis=1)


def portions_of(number_of, total, limit, lean, full):
    weights = [(1 << 20) // math.isqrt(grade ** lean) + 1 for grade in range(1, number_of + 1)]
    largest = limit if full else min(limit, max(-(-total // number_of), total * weights[0] // sum(weights)))
    least = 1 if total - largest >= number_of - 1 else 0
    counts, spare = [largest] + [least] * (number_of - 1), total - largest - least * (number_of - 1)
    while spare > 0:
        movable = [i for i in range(1, number_of) if counts[i] < largest] or [i for i in range(1, number_of) if counts[i] < limit]
        whole, left = sum([weights[i] for i in movable]), spare
        for i in movable:
            addition = min(limit - counts[i], max(1, left * weights[i] // whole), spare)
            counts[i] = counts[i] + addition
            spare = spare - addition
    return np.array(counts)


def bell_draw(own_key, extent, width, most, shards=(), kind=jnp.bfloat16):
    entries = jax.random.normal(own_key, extent, jnp.float32) * width
    if len(shards) > 0:
        entries = block_scale(own_key, extent, shards, -0.22, 0.18) * entries
    return jnp.clip(entries, min=-most, max=most).astype(kind)


def setup_inputs(seed: int = 0) -> dict:
    arg_keys = jax.random.split(jax.random.key(seed), 16)
    pool_input = draw_pool_input(jax.random.fold_in(arg_keys[15], 71), 0)
    documents = jnp.searchsorted(jnp.cumsum(uneven(arg_keys[1], DOCS, TOKENS, DOC_MAX, 2)), jnp.arange(TOKENS), side="right").astype(jnp.int32)
    residual = bell_draw(arg_keys[2], (TOKENS, D), 1.0, 6.0, ((0, 128),))
    group_weights = bell_draw(arg_keys[3], (POOL_GROUPS, GROUP_DIM, GROUP_DIM), GROUP_DIM ** -0.5, 0.75)
    pool_gain = jnp.clip(1.0 + 0.18 * jax.random.normal(arg_keys[4], (POOL_WIDTH,), jnp.float32), 0.099609375, 1.8984375).astype(jnp.bfloat16)
    output_weight = bell_draw(arg_keys[5], (POOL_WIDTH, D), POOL_WIDTH ** -0.5, 0.25)
    mixer_gain = jnp.clip(1.0 + 0.18 * jax.random.normal(arg_keys[6], (D,), jnp.float32), 0.099609375, 1.8984375).astype(jnp.bfloat16)
    routed_gain = jnp.clip(1.0 + 0.18 * jax.random.normal(arg_keys[7], (D,), jnp.float32), 0.099609375, 1.8984375).astype(jnp.bfloat16)
    final_gain = jnp.clip(1.0 + 0.18 * jax.random.normal(arg_keys[8], (D,), jnp.float32), 0.099609375, 1.8984375).astype(jnp.bfloat16)
    chosen_group_keys = jax.random.split(jax.random.fold_in(arg_keys[9], 1), TOKENS // ROWS)
    chosen_group_turns = jax.random.permutation(jax.random.fold_in(arg_keys[9], 3), TOKENS // ROWS)
    chosen_group = jax.vmap(lambda own, number: routed_block(jax.random.fold_in(arg_keys[9], 2), own, number, ROWS, GROUPS, 1, CAP, 1))(chosen_group_keys, chosen_group_turns).reshape((TOKENS, 1))
    chosen_experts = choose_distinct(arg_keys[10], TOKENS, EPG, TOPK, 0)
    expert_share = jnp.clip(0.099609375 + 0.9003906 * jax.random.uniform(arg_keys[11], (TOKENS, TOPK), jnp.float32) ** block_scale(arg_keys[11], (TOKENS, TOPK), ((0, 128),), -0.2, 0.2), 0.099609375, 1.0).astype(jnp.bfloat16)
    expert_gate = bell_draw(arg_keys[12], (EXPERTS, D, FFE), D ** -0.5, 0.125, ((0, 64), (2, 2)))
    expert_up = bell_draw(arg_keys[13], (EXPERTS, D, FFE), D ** -0.5, 0.125, ((0, 64), (2, 2)))
    expert_down = bell_draw(arg_keys[14], (EXPERTS, FFE, D), FFE ** -0.5, 0.1875, ((0, 64), (1, 2)))
    return {"pool_input": pool_input, "documents": documents, "residual": residual, "group_weights": group_weights, "pool_gain": pool_gain, "output_weight": output_weight, "mixer_gain": mixer_gain, "routed_gain": routed_gain, "final_gain": final_gain, "chosen_group": chosen_group, "chosen_experts": chosen_experts, "expert_share": expert_share, "expert_gate": expert_gate, "expert_up": expert_up, "expert_down": expert_down}


EPSILON = 1e-06
row_block = 64

def rms_scale(values, gain):
    return values * lax.rsqrt(lax.optimization_barrier(jnp.mean(values * values, axis=-1, keepdims=True)) + EPSILON) * gain.astype(jnp.float32)

def expert_rows(block_in, block_share, block_group, expert_gate, expert_up, expert_down):
    total = jnp.zeros(block_in.shape, jnp.float32)
    for block_part in range(N_TP):
        start = block_part * FFE_PART
        finish = start + FFE_PART
        part_sum = jnp.zeros(block_in.shape, jnp.float32)
        for expert in range(EPG):
            chosen = block_group * EPG + expert
            gate_full = lax.dynamic_index_in_dim(expert_gate, chosen, 0, keepdims=False)
            up_full = lax.dynamic_index_in_dim(expert_up, chosen, 0, keepdims=False)
            down_full = lax.dynamic_index_in_dim(expert_down, chosen, 0, keepdims=False)
            gate = jnp.dot(block_in, gate_full[:, start:finish], preferred_element_type=jnp.float32)
            upper = jnp.dot(block_in, up_full[:, start:finish], preferred_element_type=jnp.float32)
            hidden = (jax.nn.silu(gate) * upper).astype(jnp.bfloat16)
            product = jnp.dot(hidden, down_full[start:finish], preferred_element_type=jnp.float32)
            part_sum = part_sum + product * block_share[:, expert:expert + 1]
        total = total + lax.optimization_barrier(part_sum.astype(jnp.bfloat16)).astype(jnp.float32)
    return total.astype(jnp.bfloat16)

def reference(pool_input, documents, residual, group_weights, pool_gain, output_weight, mixer_gain, routed_gain, final_gain, chosen_group, chosen_experts, expert_share, expert_gate, expert_up, expert_down):
    values = pool_input.astype(jnp.float32)
    positions = jnp.arange(TOKENS, dtype=jnp.int32)
    doc_count = jax.ops.segment_sum(jnp.ones((TOKENS,), jnp.int32), documents, num_segments=DOCS)
    doc_begin = jnp.cumsum(doc_count) - doc_count
    begin = doc_begin[documents]
    finish = begin + doc_count[documents]
    doc_count_f = doc_count.astype(jnp.float32)
    prefix = jnp.concatenate([jnp.zeros((1, POOL_WIDTH), jnp.float32), jnp.cumsum(values, axis=0)], axis=0)
    windows = (WIN_S, WIN_M, WIN_L)
    pieces = []
    for group in range(POOL_GROUPS):
        start = group * GROUP_DIM
        own = values[:, start:start + GROUP_DIM]
        level = group % 4
        if level < 3:
            half_width = windows[level] // 2
            low = jnp.maximum(positions - half_width, begin)
            high = jnp.minimum(positions + half_width, finish)
            window_sum = prefix[high][:, start:start + GROUP_DIM] - prefix[low][:, start:start + GROUP_DIM]
            window_mean = window_sum / (high - low).astype(jnp.float32)[:, None]
        else:
            doc_sums = jax.ops.segment_sum(own, documents, num_segments=DOCS)
            window_mean = doc_sums[documents] / doc_count_f[documents][:, None]
        pool_diff = (window_mean - own).astype(jnp.bfloat16)
        pieces.append(jnp.dot(pool_diff, group_weights[group], preferred_element_type=jnp.float32))
    pooled = (jnp.concatenate(pieces, axis=1) * pool_gain.astype(jnp.float32)).astype(jnp.bfloat16)
    mixed = jnp.dot(pooled, output_weight, preferred_element_type=jnp.float32)
    stream = (residual.astype(jnp.float32) + rms_scale(mixed, mixer_gain)).astype(jnp.bfloat16)
    stream_f = lax.optimization_barrier(stream).astype(jnp.float32)
    normed = rms_scale(stream_f, routed_gain).astype(jnp.bfloat16)
    group_ids = chosen_group[:, 0]
    picked = (chosen_experts[:, :, None] == jnp.arange(EPG, dtype=jnp.int32)[None, None, :]).astype(jnp.float32)
    shares = lax.optimization_barrier(jnp.sum(expert_share.astype(jnp.float32)[:, :, None] * picked, axis=1))
    order = jnp.argsort(group_ids, stable=True).astype(jnp.int32)
    group_count = jax.ops.segment_sum(jnp.ones((TOKENS,), jnp.int32), group_ids, num_segments=GROUPS)
    padded_count = (group_count + row_block - 1) // row_block * row_block
    pad_end = jnp.cumsum(padded_count)
    pad_begin = pad_end - padded_count
    group_begin = jnp.cumsum(group_count) - group_count
    sorted_group = group_ids[order]
    dest = (pad_begin[sorted_group] + positions - group_begin[sorted_group]).astype(jnp.int32)
    block_total = (TOKENS + GROUPS * (row_block - 1)) // row_block + 1
    row_token = jnp.zeros((block_total * row_block,), jnp.int32).at[dest].set(order)
    row_live = jnp.zeros((block_total * row_block,), jnp.float32).at[dest].set(1.0)
    block_group = jnp.clip(jnp.searchsorted(pad_end, jnp.arange(block_total, dtype=jnp.int32) * row_block, side='right'), 0, GROUPS - 1).astype(jnp.int32)
    block_in = normed[row_token].reshape(block_total, row_block, D)
    block_share = (shares[row_token] * row_live[:, None]).reshape(block_total, row_block, EPG)

    def serve(item):
        return expert_rows(item[0], item[1], item[2], expert_gate, expert_up, expert_down)
    results = lax.map(serve, (block_in, block_share, block_group)).reshape(block_total * row_block, D)
    token_slot = jnp.zeros((TOKENS,), jnp.int32).at[order].set(dest)
    expert_out = results[token_slot]
    return (stream_f + rms_scale(expert_out.astype(jnp.float32), final_gain)).astype(jnp.bfloat16)
```

```python
import jax
import jax.numpy as jnp
from jax import lax
from jax.experimental import pallas as pl
from jax.experimental.pallas import tpu as pltpu
from jax.sharding import PartitionSpec as P

EPSILON = 1e-06
F32 = jnp.float32
BF16 = jnp.bfloat16
LANES = 128
HIGHEST = lax.Precision.HIGHEST
VMEM = pl.BlockSpec(memory_space=pltpu.VMEM)
ANY = pl.BlockSpec(memory_space=pl.ANY)
DOCS = 16


def dot(a, b, dims=((1,), (0,)), precision=None):
    return lax.dot_general(a, b, (dims, ((), ())), precision=precision, preferred_element_type=F32)


def call(body, out_shape, operands, flops, scratch=(), specs=None, name=None):
    moved = sum(o.size * o.dtype.itemsize for o in operands)
    outs = [jax.ShapeDtypeStruct(s, d) for s, d in out_shape]
    return pl.pallas_call(
        body,
        out_shape=outs,
        in_specs=specs or [VMEM] * len(operands),
        out_specs=[VMEM] * len(outs),
        scratch_shapes=list(scratch),
        cost_estimate=pl.CostEstimate(flops=flops, bytes_accessed=moved, transcendentals=0),
        compiler_params=pltpu.CompilerParams(vmem_limit_bytes=60 * 1024 * 1024),
        name=name,
    )(*operands)


def lane_iota(shape):
    return lax.broadcasted_iota(jnp.int32, shape, 1)


def row_iota(shape):
    return lax.broadcasted_iota(jnp.int32, shape, 0)


def swap_halves(v):
    return pltpu.roll(v, LANES // 2, 1)


def docs_kernel(x_ref, docs_ref, out_ref):
    docs = docs_ref[...]
    first = jnp.min(docs)
    last = jnp.max(docs)
    rows = x_ref.shape[0]
    pick = row_iota((8, rows))
    mask = ((pick == 0) & (docs == first)) | ((pick == 1) & (docs == last))
    mask = mask.astype(F32)
    sums = dot(mask.astype(BF16), x_ref[:, LANES : 2 * LANES])
    counts = jnp.sum(mask, axis=1, keepdims=True)
    lane = lane_iota((1, LANES))
    data = jnp.where(lane < LANES // 2, swap_halves(sums)[0:1], sums[1:2])
    meta = jnp.where(
        lane == 0,
        first.astype(F32),
        jnp.where(
            lane == 1,
            last.astype(F32),
            jnp.where(lane == 2, counts[0:1], jnp.where(lane == 3, counts[1:2], 0.0)),
        ),
    )
    both = jnp.where(row_iota(out_ref.shape) % 2 == 0, data, meta)
    out_ref[...] = both


def windows_kernel(
    own_ref,
    other_ref,
    halo_a_ref,
    halo_b_ref,
    docs_ref,
    group_ref,
    experts_ref,
    share_ref,
    diff_ref,
    x3_ref,
    local_ref,
    slot_ref,
    aux_ref,
    x_scr,
    tag_scr,
):
    t = lax.axis_index("tp")
    chip_rows, part = own_ref.shape
    rows = chip_rows // 2
    halo = rows
    span = chip_rows + halo
    docs = docs_ref[...]

    @pl.when(t == 0)
    def _():
        x_scr[halo:, :part] = own_ref[...]
        x_scr[halo:, part:] = other_ref[...]
        x_scr[:halo, :part] = halo_a_ref[:halo, :]
        x_scr[:halo, part:] = halo_b_ref[...]
        tag_scr[:, halo:] = docs.astype(F32) + 1.0
        tag_scr[:, :halo] = halo_a_ref[halo : halo + 1, :].astype(F32)

    @pl.when(t == 1)
    def _():
        x_scr[:chip_rows, part:] = own_ref[...]
        x_scr[:chip_rows, :part] = other_ref[...]
        x_scr[chip_rows:, part:] = halo_a_ref[:halo, :]
        x_scr[chip_rows:, :part] = halo_b_ref[...]
        tag_scr[:, :chip_rows] = docs.astype(F32) + 1.0
        tag_scr[:, chip_rows:] = halo_a_ref[halo : halo + 1, :].astype(F32)

    tags = tag_scr[...]
    hot = (tags == (row_iota((DOCS, span)) + 1).astype(F32)).astype(BF16)
    center = hot[:, halo : halo + rows]
    same = dot(center, hot, ((0,), (0,))) > 0.5
    offset = lane_iota((rows, span)) - halo - row_iota((rows, span))
    x = x_scr[...]
    xc = x_scr[halo : halo + rows, :].astype(F32)
    level = (lane_iota((rows, 2 * part)) // 64) % 4
    diff = xc
    for k in range(3):
        half = chip_rows * (1 << k) // 8
        mask = (same & (offset >= -half) & (offset < half)).astype(F32)
        sums = dot(mask.astype(BF16), x)
        sizes = jnp.sum(mask, axis=1, keepdims=True)
        diff = jnp.where(level == k, sums / sizes - xc, diff)
    diff_ref[...] = diff.astype(BF16)
    lane = lane_iota((rows, LANES))
    x3_ref[...] = jnp.where(
        lane < LANES // 2, swap_halves(xc[:, LANES : 2 * LANES]), xc[:, 3 * LANES : 4 * LANES]
    ).astype(BF16)

    chip_hot = docs == row_iota((DOCS, chip_rows))
    chip_hot = chip_hot.astype(F32)
    own_sum = dot(chip_hot.astype(BF16), own_ref[:, LANES : 2 * LANES])
    other_sum = dot(chip_hot.astype(BF16), other_ref[:, LANES : 2 * LANES])
    low = jnp.where(t == 0, own_sum, other_sum)
    high = jnp.where(t == 0, other_sum, own_sum)
    lane = lane_iota((DOCS, LANES))
    local_ref[:, :LANES] = jnp.where(lane < LANES // 2, swap_halves(low), high)
    local_ref[:, LANES:] = jnp.broadcast_to(
        jnp.sum(chip_hot, axis=1, keepdims=True), (DOCS, LANES)
    )

    slots = slot_ref.shape[1]
    groups = slots // 8
    ids = group_ref[...]
    member = (ids == lane_iota((rows, LANES))).astype(F32)
    earlier = (lane_iota((rows, rows)) < row_iota((rows, rows))).astype(F32).astype(BF16)
    ranks = dot(earlier, member.astype(BF16)) * member
    rank = jnp.sum(ranks, axis=1, keepdims=True).astype(jnp.int32)
    slot = ids * (slots // groups) + rank
    slot_ref[...] = (lane_iota((rows, slots)) == slot).astype(F32).astype(BF16)
    aux = jnp.zeros((rows, LANES), F32)
    lane = lane_iota((rows, LANES))
    for k in range(experts_ref.shape[1]):
        chosen = experts_ref[:, k : k + 1]
        aux = aux + jnp.where(lane == chosen, share_ref[:, k : k + 1].astype(F32), 0.0)
    aux_ref[...] = aux.astype(BF16)


def inverse_rms(v):
    return lax.rsqrt(jnp.mean(v * v, axis=-1, keepdims=True) + EPSILON)


def mixer_kernel(
    info_ref,
    local_ref,
    docs_ref,
    diff_ref,
    x3_ref,
    weights_ref,
    gain_ref,
    output_ref,
    residual_ref,
    mixer_gain_ref,
    routed_gain_ref,
    slot_ref,
    aux_ref,
    send_ref,
    stream_ref,
):
    t = lax.axis_index("tp")
    rows = diff_ref.shape[0]
    devices = info_ref.shape[0] // 2
    data = info_ref[pl.ds(0, devices, stride=2), :]
    meta = info_ref[pl.ds(1, devices, stride=2), :]
    doc = lane_iota((devices, LANES)).astype(F32)
    even = row_iota((devices, LANES)) % 2 == 0
    first_id, last_id = meta[:, 0:1], meta[:, 1:2]
    is_first = doc == first_id
    is_last = (doc == last_id) & (last_id != first_id)

    def total(mask, values):
        return dot(mask.astype(F32), values, ((0,), (0,)), HIGHEST)[:DOCS]

    first_even = is_first & even
    last_even = is_last & even
    low = total(first_even, data) + swap_halves(total(last_even, data))
    high = swap_halves(total(is_first & ~even, data)) + total(is_last & ~even, data)
    lane = lane_iota((DOCS, LANES))
    sums = jnp.where(lane < LANES // 2, low, high)
    counts = total(first_even, meta)[:, 2:3] + total(last_even, meta)[:, 3:4]
    docs = docs_ref[...]
    here = row_iota((DOCS, LANES))
    inside = (here > jnp.min(docs)) & (here < jnp.max(docs))
    sums = jnp.where(inside, local_ref[:, :LANES], sums)
    counts = jnp.where(inside, local_ref[:, LANES:], counts)
    means = sums / jnp.maximum(counts, 1.0)
    mine = jnp.where(t == 0, docs[:, :rows], docs[:, rows:])
    hot = (mine == row_iota((DOCS, rows))).astype(F32)
    doc_mean = dot(hot, means, ((0,), (0,)), HIGHEST)
    diff3 = doc_mean - x3_ref[...].astype(F32)
    half = lane_iota((rows, LANES)) < LANES // 2
    group_dim = weights_ref.shape[1]
    spread = (lane_iota((group_dim, LANES)) % group_dim == row_iota((group_dim, LANES))).astype(F32)
    spread = spread.astype(BF16)
    mixed = None
    for k in range(4):
        cols = slice(k * LANES, (k + 1) * LANES)
        diff = diff_ref[:, cols]
        if k % 2 == 1:
            wide = swap_halves(diff3) if k == 1 else diff3
            diff = jnp.where(half, diff.astype(F32), wide).astype(BF16)
        block = dot(
            jnp.concatenate([weights_ref[2 * k], weights_ref[2 * k + 1]], axis=0), spread
        )
        keep = (row_iota((LANES, LANES)) // group_dim) == (lane_iota((LANES, LANES)) // group_dim)
        block = jnp.where(keep, block, 0.0).astype(BF16)
        pooled = (dot(diff, block) * gain_ref[:, cols].astype(F32)).astype(BF16)
        part = dot(pooled, output_ref[cols, :])
        mixed = part if mixed is None else mixed + part
    stream = (
        residual_ref[...].astype(F32)
        + mixed * inverse_rms(mixed) * mixer_gain_ref[...].astype(F32)
    ).astype(BF16)
    stream_ref[...] = stream
    wide = stream.astype(F32)
    normed = (wide * inverse_rms(wide) * routed_gain_ref[...].astype(F32)).astype(BF16)
    slot = slot_ref[...]
    width = normed.shape[1]
    send_ref[:, :width] = dot(slot, normed, ((0,), (0,))).astype(BF16)
    send_ref[:, width:] = dot(slot, aux_ref[...], ((0,), (0,))).astype(BF16)


def experts_kernel(
    rows_ref,
    gate_ref,
    up_ref,
    down_ref,
    gate2_ref,
    up2_ref,
    down2_ref,
    out_ref,
    gates,
    ups,
    downs,
    acc,
    sems,
):
    experts = gate_ref.shape[0]
    width = out_ref.shape[1]
    tile = 512
    steps = 2 * experts
    sources = [(gate_ref, up_ref, down_ref), (gate2_ref, up2_ref, down2_ref)]
    buffers = (gates, ups, downs)

    def copies(step):
        part, expert = step // experts, step % experts
        return [
            pltpu.make_async_copy(
                sources[part][k].at[expert], buffers[k].at[step % 2], sems.at[k, step % 2]
            )
            for k in range(3)
        ]

    for c in copies(0):
        c.start()
    x = rows_ref[:, :width]
    shares = rows_ref[:, width:].astype(F32)
    for step in range(steps):
        slot = step % 2
        expert = step % experts
        if step + 1 < steps:
            for c in copies(step + 1):
                c.start()
        waits = copies(step)
        waits[0].wait()
        gate = dot(x, gates[slot])
        waits[1].wait()
        upper = dot(x, ups[slot])
        hidden = (gate / (1.0 + jnp.exp(-gate)) * upper).astype(BF16)
        waits[2].wait()
        share = shares[:, expert : expert + 1]
        for j in range(0, width, tile):
            cols = slice(j, j + tile)
            value = dot(hidden, downs[slot, :, cols]) * share
            if expert > 0:
                value = acc[:, cols] + value
            if expert + 1 < experts:
                acc[:, cols] = value
            elif step < experts:
                out_ref[:, cols] = value.astype(BF16)
            else:
                out_ref[:, cols] = (
                    out_ref[:, cols].astype(F32) + value.astype(BF16).astype(F32)
                ).astype(BF16)


def final_kernel(back_ref, slot_ref, stream_ref, gain_ref, out_ref):
    value = dot(slot_ref[...], back_ref[...])
    out_ref[...] = (
        stream_ref[...].astype(F32) + value * inverse_rms(value) * gain_ref[...].astype(F32)
    ).astype(BF16)


def local(
    pool_input,
    documents,
    residual,
    group_weights,
    pool_gain,
    output_weight,
    mixer_gain,
    routed_gain,
    final_gain,
    chosen_group,
    chosen_experts,
    expert_share,
    expert_gate,
    expert_up,
    expert_down,
):
    chips, cores = lax.axis_size("sp"), lax.axis_size("tp")
    t = lax.axis_index("tp")
    chip_rows, part = pool_input.shape
    rows, width = residual.shape
    groups = chips
    capacity = chip_rows // groups
    slots = groups * capacity
    swap = [(0, 1), (1, 0)]
    both = ("sp", "tp")
    docs = documents.reshape(1, chip_rows)

    (info,) = call(
        docs_kernel, [((chips * cores * 2, LANES), F32)], (pool_input, docs), 10**6, name="docs"
    )
    info = lax.all_to_all(info.reshape(chips * cores, 2, LANES), both, 0, 0, tiled=True)

    same_core = [(2 * s, 2 * s + 2) for s in range(chips - 1)]
    same_core += [(2 * s + 1, 2 * s - 1) for s in range(1, chips)]
    cross_core = [(2 * s + 1, 2 * s + 2) for s in range(chips - 1)]
    cross_core += [(2 * s, 2 * s - 1) for s in range(1, chips)]
    edge_a = (1 - t) * rows
    edge_b = t * rows
    tags = (lax.dynamic_slice_in_dim(documents, edge_a, rows, 0) + 1).astype(BF16)
    halo_a = jnp.concatenate(
        [
            lax.dynamic_slice_in_dim(pool_input, edge_a, rows, 0),
            jnp.broadcast_to(tags[None, :], (16, rows)),
        ],
        axis=0,
    )
    halo_a = lax.ppermute(halo_a, both, same_core)
    halo_b = lax.ppermute(
        lax.dynamic_slice_in_dim(pool_input, edge_b, rows, 0), both, cross_core
    )
    other = lax.ppermute(pool_input, "tp", swap)
    gate2 = lax.ppermute(expert_gate, "tp", swap)
    up2 = lax.ppermute(expert_up, "tp", swap)
    down2 = lax.ppermute(expert_down, "tp", swap)

    span = chip_rows + rows
    diff, x3, local_sums, slot, aux = call(
        windows_kernel,
        [
            ((rows, 2 * part), BF16),
            ((rows, LANES), BF16),
            ((DOCS, 2 * LANES), F32),
            ((rows, slots), BF16),
            ((rows, LANES), BF16),
        ],
        (
            pool_input,
            other,
            halo_a,
            halo_b,
            docs,
            chosen_group,
            chosen_experts,
            expert_share,
        ),
        4 * 10**9,
        scratch=[pltpu.VMEM((span, 2 * part), BF16), pltpu.VMEM((1, span), F32)],
        name="windows",
    )
    send, stream = call(
        mixer_kernel,
        [((slots, width + LANES), BF16), ((rows, width), BF16)],
        (
            info.reshape(chips * cores * 2, LANES),
            local_sums,
            docs,
            diff,
            x3,
            group_weights,
            pool_gain.reshape(1, -1),
            output_weight,
            residual,
            mixer_gain.reshape(1, -1),
            routed_gain.reshape(1, -1),
            slot,
            aux,
        ),
        2 * 10**9,
        name="mixer",
    )
    arrived = lax.all_to_all(
        send.reshape(groups, capacity, width + LANES), "sp", 0, 0, tiled=True
    ).reshape(slots, width + LANES)
    hidden = expert_gate.shape[2]
    (served,) = call(
        experts_kernel,
        [((slots, width), BF16)],
        (arrived, expert_gate, expert_up, expert_down, gate2, up2, down2),
        2 * 10**10,
        scratch=[
            pltpu.VMEM((2, width, hidden), BF16),
            pltpu.VMEM((2, width, hidden), BF16),
            pltpu.VMEM((2, hidden, width), BF16),
            pltpu.VMEM((slots, width), F32),
            pltpu.SemaphoreType.DMA((3, 2)),
        ],
        specs=[VMEM] + [ANY] * 6,
        name="experts",
    )
    back = lax.all_to_all(
        served.reshape(groups, capacity, width), "sp", 0, 0, tiled=True
    ).reshape(slots, width)
    (out,) = call(
        final_kernel,
        [((rows, width), BF16)],
        (back, slot, stream, final_gain.reshape(1, -1)),
        10**9,
        name="final",
    )
    return out


def solution(mesh):
    placed = (
        P("sp", "tp"),
        P("sp"),
        P(("sp", "tp"), None),
        P(),
        P(),
        P(),
        P(),
        P(),
        P(),
        P(("sp", "tp"), None),
        P(("sp", "tp"), None),
        P(("sp", "tp"), None),
        P("sp", None, "tp"),
        P("sp", None, "tp"),
        P("sp", "tp", None),
    )
    return jax.shard_map(
        local, mesh=mesh, in_specs=placed, out_specs=P(("sp", "tp"), None), check_vma=False
    )
```

```python
import jax
import jax.numpy as jnp
from jax import lax
from jax.experimental import pallas as pl
from jax.experimental.pallas import tpu as pltpu
from jax.sharding import PartitionSpec as P


EPSILON = 1e-06
F32 = jnp.float32
BF16 = jnp.bfloat16
LANES = 128
DOCS = 16
ROOM = 55 * 1024 * 1024
HIGHEST = lax.Precision.HIGHEST
VMEM = pl.BlockSpec(memory_space=pltpu.VMEM)
ANY = pl.BlockSpec(memory_space=pl.ANY)


def dot(a, b, dims=((1,), (0,)), precision=None):
    return lax.dot_general(a, b, (dims, ((), ())), precision=precision, preferred_element_type=F32)


def call(body, out_shape, operands, flops, room=ROOM, far=True, scratch=()):
    moved = sum(o.size * o.dtype.itemsize for o in operands)
    shapes = [jax.ShapeDtypeStruct(shape, dtype) for shape, dtype in out_shape]
    count = len(operands)

    def kernel(*refs):
        sources, rest = refs[:count], refs[count:]
        held, sems = rest[-1 - count : -1], rest[-1]
        copies = [pltpu.make_async_copy(sources[k], held[k], sems.at[k]) for k in range(count)]
        for copy in copies:
            copy.start()
        body(*zip(copies, held), *rest[: -1 - count])

    buffers = [pltpu.VMEM(o.shape, o.dtype) for o in operands]
    return pl.pallas_call(
        kernel if far else body,
        out_shape=shapes,
        in_specs=[ANY if far else VMEM] * count,
        out_specs=[VMEM] * len(shapes),
        scratch_shapes=[*scratch, *buffers, pltpu.SemaphoreType.DMA((count,))] if far else scratch,
        cost_estimate=pl.CostEstimate(flops=flops, bytes_accessed=moved, transcendentals=0),
        compiler_params=pltpu.CompilerParams(vmem_limit_bytes=room),
    )(*operands)


def landed(pair):
    pair[0].wait()
    return pair[1]


def lane_iota(shape):
    return lax.broadcasted_iota(jnp.int32, shape, 1)


def row_iota(shape):
    return lax.broadcasted_iota(jnp.int32, shape, 0)


def swap_halves(v):
    return pltpu.roll(v, LANES // 2, 1)


def as_row(ref):
    wide = ref[...].astype(F32)
    return jnp.concatenate([wide[k : k + 1] for k in range(wide.shape[0])], axis=1)


def scale_pair(t, own, other):
    low = jnp.where(t == 0, own, other)
    high = jnp.where(t == 0, other, own)
    return jnp.where(lane_iota(low.shape) < LANES // 2, swap_halves(low), high)


def docs_kernel(own, docs, other, out_ref, local_ref, edge_ref):
    t = lax.axis_index("tp")
    docs = landed(docs)[...]
    first = jnp.min(docs)
    last = jnp.max(docs)
    chip_rows = docs.shape[1]
    rows = chip_rows // 2
    hot = (docs == row_iota((DOCS, chip_rows))).astype(F32)
    hot_b = hot.astype(BF16)
    own_ref = landed(own)
    other_ref = landed(other)
    part = own_ref.shape[1]
    start = pl.multiple_of((1 - t) * rows, rows)
    tags = jnp.where(t == 0, docs[:, rows:], docs[:, :rows]) + 1
    edge_ref[:rows, :part] = own_ref[pl.ds(start, rows), :]
    edge_ref[:rows, part:] = other_ref[pl.ds(start, rows), :]
    edge_ref[rows:, :rows] = jnp.broadcast_to(tags.astype(F32), (16, rows)).astype(BF16)
    edge_ref[rows:, rows:] = jnp.zeros((16, 2 * part - rows), BF16)
    own_sums = dot(hot_b, own_ref[:, LANES : 2 * LANES])
    other_sums = dot(hot_b, other_ref[:, LANES : 2 * LANES])
    sums = scale_pair(t, own_sums, other_sums)
    counts = jnp.broadcast_to(jnp.sum(hot, axis=1, keepdims=True), (DOCS, LANES))
    here = row_iota((DOCS, LANES))
    local_ref[:, :LANES] = sums
    local_ref[:, LANES : 2 * LANES] = counts
    local_ref[:, 2 * LANES :] = ((here > first) & (here < last)).astype(F32)
    lane = lane_iota((1, LANES))

    def of(doc, values):
        return jnp.sum(jnp.where(here == doc, values, 0.0), axis=0, keepdims=True)

    meta = jnp.where(lane == 0, first.astype(F32), last.astype(F32))
    meta = jnp.where(lane == 2, of(first, counts), meta)
    meta = jnp.where(lane == 3, of(last, counts), meta)
    kind = row_iota(out_ref.shape) % 4
    out_ref[...] = jnp.where(
        kind == 0, of(first, sums), jnp.where(kind == 1, of(last, sums), meta)
    )


def slots_kernel(group, experts, share, slot_ref, aux_ref):
    slots, rows = slot_ref.shape
    groups = lax.axis_size("sp")
    ids = landed(group)[...]
    member = (ids == row_iota((groups, rows))).astype(F32)
    earlier = (row_iota((rows, rows)) < lane_iota((rows, rows))).astype(F32).astype(BF16)
    ranks = dot(member.astype(BF16), earlier) * member
    rank = jnp.sum(ranks, axis=0, keepdims=True).astype(jnp.int32)
    slot = ids * (slots // groups) + rank
    place = (row_iota((slots, rows)) == slot).astype(F32).astype(BF16)
    slot_ref[...] = place
    aux = jnp.zeros((LANES, rows), F32)
    experts_ref, share_ref = landed(experts), landed(share)
    for k in range(experts_ref.shape[0]):
        chosen = experts_ref[k : k + 1, :] == row_iota((LANES, rows))
        aux = aux + jnp.where(chosen, share_ref[k : k + 1, :].astype(F32), 0.0)
    aux_ref[...] = dot(place, aux.astype(BF16), ((1,), (1,))).astype(BF16)


def windows_kernel(own, docs, other, edge, diff_ref, x3_ref, hot_ref, x_scr, tag_scr):
    t = lax.axis_index("tp")
    docs_ref = landed(docs)
    own_ref = landed(own)
    other_ref = landed(other)
    edge_ref = landed(edge)
    chip_rows, part = own_ref.shape
    rows = chip_rows // 2
    halo = rows
    span = chip_rows + halo
    tags = edge_ref[rows : rows + 1, :rows].astype(F32)

    @pl.when(t == 0)
    def _():
        x_scr[halo:, :part] = own_ref[...]
        x_scr[halo:, part:] = other_ref[...]
        x_scr[:halo, :] = edge_ref[:rows, :]
        tag_scr[:, halo:] = docs_ref[...].astype(F32) + 1.0
        tag_scr[:, :halo] = tags

    @pl.when(t == 1)
    def _():
        x_scr[:chip_rows, part:] = own_ref[...]
        x_scr[:chip_rows, :part] = other_ref[...]
        x_scr[chip_rows:, part:] = edge_ref[:rows, :part]
        x_scr[chip_rows:, :part] = edge_ref[:rows, part:]
        tag_scr[:, :chip_rows] = docs_ref[...].astype(F32) + 1.0
        tag_scr[:, chip_rows:] = tags

    hot = (tag_scr[...] == (row_iota((DOCS, span)) + 1).astype(F32)).astype(F32)
    center = hot[:, halo : halo + rows]
    hot_ref[...] = center
    same = dot(center.astype(BF16), hot.astype(BF16), ((0,), (0,))) > 0.5
    offset = lane_iota((rows, span)) - halo - row_iota((rows, span))
    x = x_scr[...]
    xc = x_scr[halo : halo + rows, :].astype(F32)
    level = (lane_iota((rows, 2 * part)) // 64) % 4
    diff = xc
    for k in range(3):
        half = chip_rows * (1 << k) // 8
        mask = (same & (offset >= -half) & (offset < half)).astype(F32)
        sums = dot(mask.astype(BF16), x)
        sizes = jnp.sum(mask, axis=1, keepdims=True)
        diff = jnp.where(level == k, sums / sizes - xc, diff)
    diff_ref[...] = diff.astype(BF16)
    lane = lane_iota((rows, LANES))
    x3_ref[...] = jnp.where(
        lane < LANES // 2, swap_halves(xc[:, LANES : 2 * LANES]), xc[:, 3 * LANES : 4 * LANES]
    ).astype(BF16)


def inverse_rms(v):
    return lax.rsqrt(jnp.mean(v * v, axis=-1, keepdims=True) + EPSILON)


def mixer_kernel(
    info,
    local_sums,
    hot,
    x3,
    diff,
    weights,
    pool_gain,
    output,
    residual,
    mixer_gain,
    routed_gain,
    slot,
    aux,
    send_ref,
    stream_ref,
):
    info_ref = landed(info)
    local_ref = landed(local_sums)
    chips = info_ref.shape[0] // 4
    firsts, lasts, meta = (info_ref[pl.ds(k, chips, stride=4), :] for k in range(3))
    doc = lane_iota((chips, LANES)).astype(F32)
    first_id, last_id = meta[:, 0:1], meta[:, 1:2]
    is_first = (doc == first_id).astype(F32)
    is_last = ((doc == last_id) & (last_id != first_id)).astype(F32)

    def total(mask, values):
        return dot(mask, values, ((0,), (0,)), HIGHEST)[:DOCS]

    sums = total(is_first, firsts) + total(is_last, lasts)
    counts = total(is_first, meta)[:, 2:3] + total(is_last, meta)[:, 3:4]
    inside = local_ref[:, 2 * LANES :] > 0.5
    sums = jnp.where(inside, local_ref[:, :LANES], sums)
    counts = jnp.where(inside, local_ref[:, LANES : 2 * LANES], counts)
    means = sums / jnp.maximum(counts, 1.0)
    doc_mean = dot(landed(hot)[...], means, ((0,), (0,)), HIGHEST)
    diff3 = doc_mean - landed(x3)[...].astype(F32)
    rows = diff3.shape[0]
    half = lane_iota((rows, LANES)) < LANES // 2
    weights_ref = landed(weights)
    gain = as_row(landed(pool_gain))
    diff_ref = landed(diff)
    dim = weights_ref.shape[1]
    spread = lane_iota((dim, LANES)) % dim == row_iota((dim, LANES))
    spread = spread.astype(F32).astype(BF16)
    keep = (row_iota((LANES, LANES)) // dim) == (lane_iota((LANES, LANES)) // dim)
    pooled = []
    for k in range(4):
        cols = slice(k * LANES, (k + 1) * LANES)
        part = diff_ref[:, cols]
        if k % 2 == 1:
            wide = swap_halves(diff3) if k == 1 else diff3
            part = jnp.where(half, part.astype(F32), wide).astype(BF16)
        pair = jnp.concatenate([weights_ref[2 * k], weights_ref[2 * k + 1]], axis=0)
        block = jnp.where(keep, dot(pair, spread), 0.0).astype(BF16)
        pooled.append((dot(part, block) * gain[:, cols]).astype(BF16))
    mixed = dot(jnp.concatenate(pooled, axis=1), landed(output)[...])
    mixer_row = as_row(landed(mixer_gain))
    routed_row = as_row(landed(routed_gain))
    stream = (
        landed(residual)[...].astype(F32) + mixed * inverse_rms(mixed) * mixer_row
    ).astype(BF16)
    stream_ref[...] = stream
    wide = stream.astype(F32)
    normed = (wide * inverse_rms(wide) * routed_row).astype(BF16)
    width = normed.shape[1]
    send_ref[:, :width] = dot(landed(slot)[...], normed).astype(BF16)
    send_ref[:, width:] = landed(aux)[...]


def experts_kernel(
    rows_ref,
    gate_ref,
    up_ref,
    down_ref,
    gate2_ref,
    up2_ref,
    down2_ref,
    out_ref,
    gates,
    ups,
    downs,
    acc,
    hidden,
    result,
    sems,
    out_sems,
):
    experts = gate_ref.shape[0]
    width = out_ref.shape[1]
    tile = 512
    units = gates.shape[2]
    steps = 2 * experts
    sources = [(gate_ref, up_ref, down_ref), (gate2_ref, up2_ref, down2_ref)]
    buffers = (gates, ups, downs)

    def copy(step, k):
        part, expert = step // experts, step % experts
        return pltpu.make_async_copy(
            sources[part][k].at[expert], buffers[k].at[step % 2], sems.at[k, step % 2]
        )

    def leave(cols, j):
        return pltpu.make_async_copy(result.at[:, cols], out_ref.at[:, cols], out_sems.at[j])

    def up_half(step, n):
        slot = step % 2
        cols = slice(n * units // 2, (n + 1) * units // 2)
        x = rows_ref[:, :width]
        gate = dot(x, gates[slot, :, cols])
        upper = dot(x, ups[slot, :, cols])
        hidden[slot, :, cols] = (gate / (1.0 + jnp.exp(-gate)) * upper).astype(BF16)

    def down_tile(step, j):
        slot, expert = step % 2, step % experts
        cols = slice(j * tile, (j + 1) * tile)
        share = rows_ref[:, width : width + LANES].astype(F32)[:, expert : expert + 1]
        value = dot(hidden[slot], downs[slot, :, cols]) * share
        if expert > 0:
            value = acc[:, cols] + value
        if expert + 1 < experts:
            acc[:, cols] = value
        elif step < experts:
            result[:, cols] = value.astype(BF16)
        else:
            result[:, cols] = (
                result[:, cols].astype(F32) + value.astype(BF16).astype(F32)
            ).astype(BF16)
            leave(cols, j).start()

    tiles = width // tile
    for k in range(3):
        copy(0, k).start()
    for step in range(steps + 1):
        if step < steps:
            copy(step, 0).wait()
            copy(step, 1).wait()
        if step > 0:
            copy(step - 1, 2).wait()
        if step + 1 < steps:
            copy(step + 1, 0).start()
            copy(step + 1, 1).start()
        for n in range(2):
            if step < steps:
                up_half(step, n)
            if step > 0:
                for j in range(n * tiles // 2, (n + 1) * tiles // 2):
                    down_tile(step - 1, j)
        if step + 1 < steps:
            copy(step + 1, 2).start()
    for j in range(tiles):
        leave(slice(j * tile, (j + 1) * tile), j).wait()


def final_kernel(gain_ref, back_ref, slot_ref, stream_ref, out_ref):
    value = dot(slot_ref[...], back_ref[...], ((0,), (0,)))
    gain = as_row(gain_ref)
    out_ref[...] = (stream_ref[...].astype(F32) + value * inverse_rms(value) * gain).astype(BF16)


def local(
    pool_input,
    documents,
    residual,
    group_weights,
    pool_gain,
    output_weight,
    mixer_gain,
    routed_gain,
    final_gain,
    chosen_group,
    chosen_experts,
    expert_share,
    expert_gate,
    expert_up,
    expert_down,
):
    chips = lax.axis_size("sp")
    chip_rows, part = pool_input.shape
    rows, width = residual.shape
    groups = chips
    capacity = chip_rows // groups
    slots = groups * capacity
    swap = [(0, 1), (1, 0)]
    both = ("sp", "tp")
    docs = documents.reshape(1, chip_rows)

    def tiles(gain):
        return gain.reshape(-1, LANES)

    other = lax.ppermute(pool_input, "tp", swap)
    gate2 = lax.ppermute(expert_gate, "tp", swap)
    up2 = lax.ppermute(expert_up, "tp", swap)
    down2 = lax.ppermute(expert_down, "tp", swap)
    slot, aux = call(
        slots_kernel,
        [((slots, rows), BF16), ((slots, LANES), BF16)],
        (chosen_group.T, chosen_experts.T, expert_share.T),
        10**8,
    )
    info, local_sums, edge = call(
        docs_kernel,
        [
            ((chips * 4, LANES), F32),
            ((DOCS, 3 * LANES), F32),
            ((rows + 16, 2 * part), BF16),
        ],
        (pool_input, docs, other),
        10**8,
    )
    same_core = [(2 * s, 2 * s + 2) for s in range(chips - 1)]
    same_core += [(2 * s + 1, 2 * s - 1) for s in range(1, chips)]
    edge = lax.ppermute(edge, both, same_core)
    info = lax.all_to_all(info.reshape(chips, 4, LANES), "sp", 0, 0, tiled=True)

    span = chip_rows + rows
    diff, x3, hot = call(
        windows_kernel,
        [((rows, 2 * part), BF16), ((rows, LANES), BF16), ((DOCS, rows), F32)],
        (pool_input, docs, other, edge),
        10**9,
        scratch=[pltpu.VMEM((span, 2 * part), BF16), pltpu.VMEM((1, span), F32)],
    )
    send, stream = call(
        mixer_kernel,
        [((slots, width + LANES), BF16), ((rows, width), BF16)],
        (
            info.reshape(chips * 4, LANES),
            local_sums,
            hot,
            x3,
            diff,
            group_weights,
            tiles(pool_gain),
            output_weight,
            residual,
            tiles(mixer_gain),
            tiles(routed_gain),
            slot,
            aux,
        ),
        2 * 10**9,
    )
    arrived = lax.all_to_all(
        send.reshape(groups, capacity, width + LANES), "sp", 0, 0, tiled=True
    ).reshape(slots, width + LANES)
    units = expert_gate.shape[2]
    served = pl.pallas_call(
        experts_kernel,
        out_shape=jax.ShapeDtypeStruct((slots, width), BF16),
        in_specs=[VMEM] + [ANY] * 6,
        out_specs=ANY,
        scratch_shapes=[
            pltpu.VMEM((2, width, units), BF16),
            pltpu.VMEM((2, width, units), BF16),
            pltpu.VMEM((2, units, width), BF16),
            pltpu.VMEM((slots, width), F32),
            pltpu.VMEM((2, slots, units), BF16),
            pltpu.VMEM((slots, width), BF16),
            pltpu.SemaphoreType.DMA((3, 2)),
            pltpu.SemaphoreType.DMA((4,)),
        ],
        cost_estimate=pl.CostEstimate(
            flops=2 * 10**10, bytes_accessed=40 * 10**6, transcendentals=0
        ),
        compiler_params=pltpu.CompilerParams(vmem_limit_bytes=48 * 1024 * 1024),
        name="experts",
    )(arrived, expert_gate, expert_up, expert_down, gate2, up2, down2)
    back = lax.all_to_all(
        served.reshape(groups, capacity, width), "sp", 0, 0, tiled=True
    ).reshape(slots, width)
    (out,) = call(
        final_kernel,
        [((rows, width), BF16)],
        (tiles(final_gain), back, slot, stream),
        10**9,
        room=20 * 1024 * 1024,
        far=False,
    )
    return out


def solution(mesh):
    placed = (
        P("sp", "tp"),
        P("sp"),
        P(("sp", "tp"), None),
        P(),
        P(),
        P(),
        P(),
        P(),
        P(),
        P(("sp", "tp"), None),
        P(("sp", "tp"), None),
        P(("sp", "tp"), None),
        P("sp", None, "tp"),
        P("sp", None, "tp"),
        P("sp", "tp", None),
    )

    return jax.shard_map(
        local, mesh=mesh, in_specs=placed, out_specs=P(("sp", "tp"), None), check_vma=False
    )
```

```python
import jax
import jax.numpy as jnp
from jax import lax
from jax.experimental import pallas as pl
from jax.experimental.pallas import tpu as pltpu
from jax.sharding import PartitionSpec as P


EPSILON = 1e-06
F32 = jnp.float32
BF16 = jnp.bfloat16
LANES = 128
DOCS = 16
ROOM = 55 * 1024 * 1024
HIGHEST = lax.Precision.HIGHEST
VMEM = pl.BlockSpec(memory_space=pltpu.VMEM)
ANY = pl.BlockSpec(memory_space=pl.ANY)


def dot(a, b, dims=((1,), (0,)), precision=None):
    return lax.dot_general(a, b, (dims, ((), ())), precision=precision, preferred_element_type=F32)


def call(body, out_shape, operands, flops, room=ROOM, far=True, outs=VMEM, scratch=()):
    moved = sum(o.size * o.dtype.itemsize for o in operands)
    shapes = [jax.ShapeDtypeStruct(shape, dtype) for shape, dtype in out_shape]
    count = len(operands)

    def kernel(*refs):
        sources, rest = refs[:count], refs[count:]
        held, sems = rest[-1 - count : -1], rest[-1]
        copies = [pltpu.make_async_copy(sources[k], held[k], sems.at[k]) for k in range(count)]
        for copy in copies:
            copy.start()
        body(*zip(copies, held), *rest[: -1 - count])

    buffers = [pltpu.VMEM(o.shape, o.dtype) for o in operands]
    return pl.pallas_call(
        kernel if far else body,
        out_shape=shapes,
        in_specs=[ANY if far else VMEM] * count,
        out_specs=[outs] * len(shapes),
        scratch_shapes=[*scratch, *buffers, pltpu.SemaphoreType.DMA((count,))] if far else scratch,
        cost_estimate=pl.CostEstimate(flops=flops, bytes_accessed=moved, transcendentals=0),
        compiler_params=pltpu.CompilerParams(vmem_limit_bytes=room),
    )(*operands)


def landed(pair):
    pair[0].wait()
    return pair[1]


def lane_iota(shape):
    return lax.broadcasted_iota(jnp.int32, shape, 1)


def row_iota(shape):
    return lax.broadcasted_iota(jnp.int32, shape, 0)


def own_lane(shape, capacity):
    return lane_iota(shape) % capacity == row_iota(shape) % capacity


def slot_source(shape, capacity, axis):
    group = lax.broadcasted_iota(jnp.int32, shape, axis)
    slot = lax.broadcasted_iota(jnp.int32, shape, 1 - axis)
    return (group == slot // capacity).astype(F32).astype(BF16)


def swap_halves(v):
    return pltpu.roll(v, LANES // 2, 1)


def as_row(ref):
    wide = ref[...].astype(F32)
    return jnp.concatenate([wide[k : k + 1] for k in range(wide.shape[0])], axis=1)


def scale_pair(t, own, other):
    low = jnp.where(t == 0, own, other)
    high = jnp.where(t == 0, other, own)
    return jnp.where(lane_iota(low.shape) < LANES // 2, swap_halves(low), high)


def docs_kernel(own, docs, other, shares, out_ref, local_ref, edge_ref):
    t = lax.axis_index("tp")
    docs = landed(docs)[...]
    first = jnp.min(docs)
    last = jnp.max(docs)
    chip_rows = docs.shape[1]
    rows = chip_rows // 2
    hot = (docs == row_iota((DOCS, chip_rows))).astype(F32)
    hot_b = hot.astype(BF16)
    own_ref = landed(own)
    other_ref = landed(other)
    part = own_ref.shape[1]
    start = pl.multiple_of((1 - t) * rows, rows)
    tags = jnp.where(t == 0, docs[:, rows:], docs[:, :rows]) + 1
    edge_ref[:rows, :part] = own_ref[pl.ds(start, rows), :]
    edge_ref[:rows, part:] = other_ref[pl.ds(start, rows), :]
    edge_ref[rows:, :rows] = jnp.broadcast_to(tags.astype(F32), (16, rows)).astype(BF16)
    edge_ref[rows:, rows:] = jnp.zeros((16, 2 * part - rows), BF16)
    own_sums = dot(hot_b, own_ref[:, LANES : 2 * LANES])
    other_sums = dot(hot_b, other_ref[:, LANES : 2 * LANES])
    sums = scale_pair(t, own_sums, other_sums)
    counts = jnp.broadcast_to(jnp.sum(hot, axis=1, keepdims=True), (DOCS, LANES))
    here = row_iota((DOCS, LANES))
    local_ref[:, :LANES] = sums
    local_ref[:, LANES : 2 * LANES] = counts
    local_ref[:, 2 * LANES :] = ((here > first) & (here < last)).astype(F32)
    lane = lane_iota((1, LANES))

    def of(doc, values):
        return jnp.sum(jnp.where(here == doc, values, 0.0), axis=0, keepdims=True)

    meta = jnp.where(lane == 0, first.astype(F32), last.astype(F32))
    meta = jnp.where(lane == 2, of(first, counts), meta)
    meta = jnp.where(lane == 3, of(last, counts), meta)
    kind = row_iota(out_ref.shape) % 4
    out_ref[...] = jnp.where(
        kind == 0, of(first, sums), jnp.where(kind == 1, of(last, sums), meta)
    )
    out_ref[pl.ds(3, out_ref.shape[0] // 4, stride=4), :] = landed(shares)[...]


def slots_kernel(group, experts, share, slot_ref, shares_ref):
    slots, rows = slot_ref.shape
    groups = lax.axis_size("sp")
    ids = landed(group)[...]
    member = (ids == row_iota((groups, rows))).astype(F32)
    earlier = (row_iota((rows, rows)) < lane_iota((rows, rows))).astype(F32).astype(BF16)
    ranks = dot(member.astype(BF16), earlier) * member
    rank = jnp.sum(ranks, axis=0, keepdims=True).astype(jnp.int32)
    slot = ids * (slots // groups) + rank
    place = (row_iota((slots, rows)) == slot).astype(F32).astype(BF16)
    slot_ref[...] = place
    capacity = slots // groups
    spread = jnp.zeros((LANES, rows), F32)
    experts_ref, share_ref = landed(experts), landed(share)
    for k in range(experts_ref.shape[0]):
        chosen = experts_ref[k : k + 1, :] == row_iota((LANES, rows)) // capacity
        spread = spread + jnp.where(chosen, share_ref[k : k + 1, :].astype(F32), 0.0)
    each = dot(place, spread.astype(BF16), ((1,), (1,)))
    each = jnp.where(own_lane((slots, LANES), capacity), each, 0.0).astype(BF16)
    shares_ref[...] = dot(slot_source((groups, slots), capacity, 0), each)


def windows_kernel(own, docs, other, edge, diff_ref, x3_ref, hot_ref, x_scr, tag_scr):
    t = lax.axis_index("tp")
    docs_ref = landed(docs)
    own_ref = landed(own)
    other_ref = landed(other)
    edge_ref = landed(edge)
    chip_rows, part = own_ref.shape
    rows = chip_rows // 2
    halo = rows
    span = chip_rows + halo
    tags = edge_ref[rows : rows + 1, :rows].astype(F32)

    @pl.when(t == 0)
    def _():
        x_scr[halo:, :part] = own_ref[...]
        x_scr[halo:, part:] = other_ref[...]
        x_scr[:halo, :] = edge_ref[:rows, :]
        tag_scr[:, halo:] = docs_ref[...].astype(F32) + 1.0
        tag_scr[:, :halo] = tags

    @pl.when(t == 1)
    def _():
        x_scr[:chip_rows, part:] = own_ref[...]
        x_scr[:chip_rows, :part] = other_ref[...]
        x_scr[chip_rows:, part:] = edge_ref[:rows, :part]
        x_scr[chip_rows:, :part] = edge_ref[:rows, part:]
        tag_scr[:, :chip_rows] = docs_ref[...].astype(F32) + 1.0
        tag_scr[:, chip_rows:] = tags

    hot = (tag_scr[...] == (row_iota((DOCS, span)) + 1).astype(F32)).astype(F32)
    center = hot[:, halo : halo + rows]
    hot_ref[...] = center
    same = dot(center.astype(BF16), hot.astype(BF16), ((0,), (0,))) > 0.5
    offset = lane_iota((rows, span)) - halo - row_iota((rows, span))
    x = x_scr[...]
    xc = x_scr[halo : halo + rows, :].astype(F32)
    level = (lane_iota((rows, 2 * part)) // 64) % 4
    diff = xc
    for k in range(3):
        half = chip_rows * (1 << k) // 8
        mask = (same & (offset >= -half) & (offset < half)).astype(F32)
        sums = dot(mask.astype(BF16), x)
        sizes = jnp.sum(mask, axis=1, keepdims=True)
        diff = jnp.where(level == k, sums / sizes - xc, diff)
    diff_ref[...] = diff.astype(BF16)
    lane = lane_iota((rows, LANES))
    x3_ref[...] = jnp.where(
        lane < LANES // 2, swap_halves(xc[:, LANES : 2 * LANES]), xc[:, 3 * LANES : 4 * LANES]
    ).astype(BF16)


def inverse_rms(v):
    return lax.rsqrt(jnp.mean(v * v, axis=-1, keepdims=True) + EPSILON)


def mixer_kernel(
    info,
    local_sums,
    hot,
    x3,
    diff,
    weights,
    pool_gain,
    output,
    residual,
    mixer_gain,
    routed_gain,
    slot,
    send_out,
    stream_out,
    send_ref,
    stream_ref,
    out_sems,
):
    info_ref = landed(info)
    local_ref = landed(local_sums)
    chips = info_ref.shape[0] // 4
    firsts, lasts, meta = (info_ref[pl.ds(k, chips, stride=4), :] for k in range(3))
    doc = lane_iota((chips, LANES)).astype(F32)
    first_id, last_id = meta[:, 0:1], meta[:, 1:2]
    is_first = (doc == first_id).astype(F32)
    is_last = ((doc == last_id) & (last_id != first_id)).astype(F32)

    def total(mask, values):
        return dot(mask, values, ((0,), (0,)), HIGHEST)[:DOCS]

    sums = total(is_first, firsts) + total(is_last, lasts)
    counts = total(is_first, meta)[:, 2:3] + total(is_last, meta)[:, 3:4]
    inside = local_ref[:, 2 * LANES :] > 0.5
    sums = jnp.where(inside, local_ref[:, :LANES], sums)
    counts = jnp.where(inside, local_ref[:, LANES : 2 * LANES], counts)
    means = sums / jnp.maximum(counts, 1.0)
    doc_mean = dot(landed(hot)[...], means, ((0,), (0,)), HIGHEST)
    diff3 = doc_mean - landed(x3)[...].astype(F32)
    rows = diff3.shape[0]
    half = lane_iota((rows, LANES)) < LANES // 2
    weights_ref = landed(weights)
    gain = as_row(landed(pool_gain))
    diff_ref = landed(diff)
    dim = weights_ref.shape[1]
    spread = lane_iota((dim, LANES)) % dim == row_iota((dim, LANES))
    spread = spread.astype(F32).astype(BF16)
    keep = (row_iota((LANES, LANES)) // dim) == (lane_iota((LANES, LANES)) // dim)
    pooled = []
    for k in range(4):
        cols = slice(k * LANES, (k + 1) * LANES)
        part = diff_ref[:, cols]
        if k % 2 == 1:
            wide = swap_halves(diff3) if k == 1 else diff3
            part = jnp.where(half, part.astype(F32), wide).astype(BF16)
        pair = jnp.concatenate([weights_ref[2 * k], weights_ref[2 * k + 1]], axis=0)
        block = jnp.where(keep, dot(pair, spread), 0.0).astype(BF16)
        pooled.append((dot(part, block) * gain[:, cols]).astype(BF16))
    mixed = dot(jnp.concatenate(pooled, axis=1), landed(output)[...])
    mixer_row = as_row(landed(mixer_gain))
    routed_row = as_row(landed(routed_gain))
    stream = (
        landed(residual)[...].astype(F32) + mixed * inverse_rms(mixed) * mixer_row
    ).astype(BF16)
    stream_ref[...] = stream
    leaving = [pltpu.make_async_copy(stream_ref, stream_out, out_sems.at[0])]
    leaving[0].start()
    wide = stream.astype(F32)
    normed = (wide * inverse_rms(wide) * routed_row).astype(BF16)
    width = normed.shape[1]
    place = landed(slot)[...]
    for k in range(4):
        cols = slice(k * width // 4, (k + 1) * width // 4)
        send_ref[:, cols] = dot(place, normed[:, cols]).astype(BF16)
        leaving.append(
            pltpu.make_async_copy(send_ref.at[:, cols], send_out.at[:, cols], out_sems.at[k + 1])
        )
        leaving[-1].start()
    for copy in leaving:
        copy.wait()


def experts_kernel(
    rows_ref,
    info_ref,
    gate_ref,
    up_ref,
    down_ref,
    gate2_ref,
    up2_ref,
    down2_ref,
    out_ref,
    gates,
    ups,
    downs,
    acc,
    hidden,
    result,
    info,
    shares,
    sems,
    out_sems,
    first_sems,
):
    experts = gate_ref.shape[0]
    width = out_ref.shape[1]
    tile = 512
    units = gates.shape[2]
    steps = 2 * experts
    sources = [(gate_ref, up_ref, down_ref), (gate2_ref, up2_ref, down2_ref)]
    buffers = (gates, ups, downs)

    def copy(step, k):
        part, expert = step // experts, step % experts
        return pltpu.make_async_copy(
            sources[part][k].at[expert], buffers[k].at[step % 2], sems.at[k, step % 2]
        )

    def first(k, n):
        cols = slice(n * units // 2, (n + 1) * units // 2)
        return pltpu.make_async_copy(
            sources[0][k].at[0, :, cols], buffers[k].at[0, :, cols], first_sems.at[k, n]
        )

    def leave(cols, j):
        return pltpu.make_async_copy(result.at[:, cols], out_ref.at[:, cols], out_sems.at[j])

    def up_half(step, n):
        slot = step % 2
        cols = slice(n * units // 2, (n + 1) * units // 2)
        x = rows_ref[...]
        gate = dot(x, gates[slot, :, cols])
        upper = dot(x, ups[slot, :, cols])
        hidden[slot, :, cols] = (gate / (1.0 + jnp.exp(-gate)) * upper).astype(BF16)

    def down_tile(step, j):
        slot, expert = step % 2, step % experts
        cols = slice(j * tile, (j + 1) * tile)
        share = jnp.concatenate([shares[expert]] * (tile // LANES), axis=1)
        value = dot(hidden[slot], downs[slot, :, cols]) * share
        if expert > 0:
            value = acc[:, cols] + value
        if expert + 1 < experts:
            acc[:, cols] = value
        elif step < experts:
            result[:, cols] = value.astype(BF16)
        else:
            result[:, cols] = (
                result[:, cols].astype(F32) + value.astype(BF16).astype(F32)
            ).astype(BF16)
            leave(cols, j).start()

    tiles = width // tile
    told = pltpu.make_async_copy(info_ref, info, out_sems.at[0])
    told.start()
    for n in range(2):
        first(0, n).start()
        first(1, n).start()
    copy(0, 2).start()
    told.wait()
    slots = rows_ref.shape[0]
    groups = info.shape[0] // 4
    capacity = slots // groups
    sent = info[pl.ds(3, groups, stride=4), :].astype(BF16)
    sent = dot(slot_source((slots, groups), capacity, 1), sent)
    sent = jnp.where(own_lane((slots, LANES), capacity), sent, 0.0)
    for e in range(experts):
        one = jnp.where(lane_iota((slots, LANES)) // capacity == e, sent, 0.0)
        shares[e] = jnp.broadcast_to(jnp.sum(one, axis=1, keepdims=True), (slots, LANES))
    for step in range(steps + 1):
        if 0 < step < steps:
            copy(step, 0).wait()
            copy(step, 1).wait()
        if step > 0:
            copy(step - 1, 2).wait()
        if step + 1 < steps:
            copy(step + 1, 0).start()
            copy(step + 1, 1).start()
        for n in range(2):
            if step == 0:
                first(0, n).wait()
                first(1, n).wait()
            if step < steps:
                up_half(step, n)
            if step > 0:
                for j in range(n * tiles // 2, (n + 1) * tiles // 2):
                    down_tile(step - 1, j)
        if step + 1 < steps:
            copy(step + 1, 2).start()
    for j in range(tiles):
        leave(slice(j * tile, (j + 1) * tile), j).wait()


def final_kernel(gain_ref, back_ref, slot_ref, stream_ref, out_ref, held, sems):
    gain = as_row(gain_ref)
    count = sems.shape[0]
    step = held.shape[0] // count
    leaving = []
    for k in range(count):
        rows = slice(k * step, (k + 1) * step)
        value = dot(slot_ref[:, rows], back_ref[...], ((0,), (0,)))
        held[rows, :] = (
            stream_ref[rows, :].astype(F32) + value * inverse_rms(value) * gain
        ).astype(BF16)
        leaving.append(pltpu.make_async_copy(held.at[rows], out_ref.at[rows], sems.at[k]))
        leaving[-1].start()
    for copy in leaving:
        copy.wait()


def local(
    pool_input,
    documents,
    residual,
    group_weights,
    pool_gain,
    output_weight,
    mixer_gain,
    routed_gain,
    final_gain,
    chosen_group,
    chosen_experts,
    expert_share,
    expert_gate,
    expert_up,
    expert_down,
):
    chips = lax.axis_size("sp")
    chip_rows, part = pool_input.shape
    rows, width = residual.shape
    groups = chips
    capacity = chip_rows // groups
    slots = groups * capacity
    swap = [(0, 1), (1, 0)]
    both = ("sp", "tp")
    docs = documents.reshape(1, chip_rows)

    def tiles(gain):
        return gain.reshape(-1, LANES)

    other = lax.ppermute(pool_input, "tp", swap)
    gate2 = lax.ppermute(expert_gate, "tp", swap)
    up2 = lax.ppermute(expert_up, "tp", swap)
    down2 = lax.ppermute(expert_down, "tp", swap)
    slot, shares = call(
        slots_kernel,
        [((slots, rows), BF16), ((groups, LANES), F32)],
        (chosen_group.T, chosen_experts.T, expert_share.T),
        10**8,
    )
    info, local_sums, edge = call(
        docs_kernel,
        [
            ((chips * 4, LANES), F32),
            ((DOCS, 3 * LANES), F32),
            ((rows + 16, 2 * part), BF16),
        ],
        (pool_input, docs, other, shares),
        10**8,
    )
    same_core = [(2 * s, 2 * s + 2) for s in range(chips - 1)]
    same_core += [(2 * s + 1, 2 * s - 1) for s in range(1, chips)]
    edge = lax.ppermute(edge, both, same_core)
    info = lax.all_to_all(info.reshape(chips, 4, LANES), "sp", 0, 0, tiled=True)
    info = info.reshape(chips * 4, LANES)

    span = chip_rows + rows
    diff, x3, hot = call(
        windows_kernel,
        [((rows, 2 * part), BF16), ((rows, LANES), BF16), ((DOCS, rows), F32)],
        (pool_input, docs, other, edge),
        10**9,
        scratch=[pltpu.VMEM((span, 2 * part), BF16), pltpu.VMEM((1, span), F32)],
    )
    send, stream = call(
        mixer_kernel,
        [((slots, width), BF16), ((rows, width), BF16)],
        (
            info,
            local_sums,
            hot,
            x3,
            diff,
            group_weights,
            tiles(pool_gain),
            output_weight,
            residual,
            tiles(mixer_gain),
            tiles(routed_gain),
            slot,
        ),
        2 * 10**9,
        outs=ANY,
        scratch=[
            pltpu.VMEM((slots, width), BF16),
            pltpu.VMEM((rows, width), BF16),
            pltpu.SemaphoreType.DMA((5,)),
        ],
    )
    arrived = lax.all_to_all(
        send.reshape(groups, capacity, width), "sp", 0, 0, tiled=True
    ).reshape(slots, width)
    units = expert_gate.shape[2]
    served = pl.pallas_call(
        experts_kernel,
        out_shape=jax.ShapeDtypeStruct((slots, width), BF16),
        in_specs=[VMEM] + [ANY] * 7,
        out_specs=ANY,
        scratch_shapes=[
            pltpu.VMEM((2, width, units), BF16),
            pltpu.VMEM((2, width, units), BF16),
            pltpu.VMEM((2, units, width), BF16),
            pltpu.VMEM((slots, width), F32),
            pltpu.VMEM((2, slots, units), BF16),
            pltpu.VMEM((slots, width), BF16),
            pltpu.VMEM((chips * 4, LANES), F32),
            pltpu.VMEM((expert_gate.shape[0], slots, LANES), F32),
            pltpu.SemaphoreType.DMA((3, 2)),
            pltpu.SemaphoreType.DMA((4,)),
            pltpu.SemaphoreType.DMA((2, 2)),
        ],
        cost_estimate=pl.CostEstimate(
            flops=2 * 10**10, bytes_accessed=40 * 10**6, transcendentals=0
        ),
        compiler_params=pltpu.CompilerParams(vmem_limit_bytes=48 * 1024 * 1024),
        name="experts",
    )(arrived, info, expert_gate, expert_up, expert_down, gate2, up2, down2)
    back = lax.all_to_all(
        served.reshape(groups, capacity, width), "sp", 0, 0, tiled=True
    ).reshape(slots, width)
    (out,) = call(
        final_kernel,
        [((rows, width), BF16)],
        (tiles(final_gain), back, slot, stream),
        10**9,
        room=20 * 1024 * 1024,
        far=False,
        outs=ANY,
        scratch=[pltpu.VMEM((rows, width), BF16), pltpu.SemaphoreType.DMA((2,))],
    )
    return out


def solution(mesh):
    placed = (
        P("sp", "tp"),
        P("sp"),
        P(("sp", "tp"), None),
        P(),
        P(),
        P(),
        P(),
        P(),
        P(),
        P(("sp", "tp"), None),
        P(("sp", "tp"), None),
        P(("sp", "tp"), None),
        P("sp", None, "tp"),
        P("sp", None, "tp"),
        P("sp", "tp", None),
    )

    return jax.shard_map(
        local, mesh=mesh, in_specs=placed, out_specs=P(("sp", "tp"), None), check_vma=False
    )
```

```python
import jax
import jax.numpy as jnp
from jax import lax
from jax.experimental import pallas as pl
from jax.experimental.pallas import tpu as pltpu
from jax.sharding import PartitionSpec as P


EPSILON = 1e-06
F32 = jnp.float32
BF16 = jnp.bfloat16
LANES = 128
DOCS = 16
ROOM = 55 * 1024 + 256
HIGHEST = lax.Precision.HIGHEST
VMEM = pl.BlockSpec(memory_space=pltpu.VMEM)
ANY = pl.BlockSpec(memory_space=pl.ANY)


def dot(a, b, dims=((1,), (0,)), precision=None):
    return lax.dot_general(a, b, (dims, ((), ())), precision=precision, preferred_element_type=F32)


def call(body, out_shape, far, flops, near=(), spare=0, outs=VMEM, scratch=()):
    moved = sum(o.size * o.dtype.itemsize for o in (*far, *near))
    shapes = [jax.ShapeDtypeStruct(shape, dtype) for shape, dtype in out_shape]
    count = len(far)

    def kernel(*refs):
        sources, rest = refs[:count], refs[count:]
        held, sems = rest[-1 - count : -1], rest[-1]
        copies = [pltpu.make_async_copy(sources[k], held[k], sems.at[k]) for k in range(count)]
        for copy in copies:
            copy.start()
        body(*zip(copies, held), *rest[: -1 - count])

    buffers = [pltpu.VMEM(o.shape, o.dtype) for o in far]
    return pl.pallas_call(
        kernel if far else body,
        out_shape=shapes,
        in_specs=[ANY] * count + [VMEM] * len(near),
        out_specs=[outs] * len(shapes),
        scratch_shapes=[*scratch, *buffers, pltpu.SemaphoreType.DMA((count,))] if far else scratch,
        cost_estimate=pl.CostEstimate(flops=flops, bytes_accessed=moved, transcendentals=0),
        compiler_params=pltpu.CompilerParams(vmem_limit_bytes=(ROOM - spare) * 1024),
    )(*far, *near)


def landed(pair):
    pair[0].wait()
    return pair[1]


def lane_iota(shape):
    return lax.broadcasted_iota(jnp.int32, shape, 1)


def row_iota(shape):
    return lax.broadcasted_iota(jnp.int32, shape, 0)


def own_lane(shape, capacity):
    return lane_iota(shape) % capacity == row_iota(shape) % capacity


def slot_source(shape, capacity, axis):
    group = lax.broadcasted_iota(jnp.int32, shape, axis)
    slot = lax.broadcasted_iota(jnp.int32, shape, 1 - axis)
    return (group == slot // capacity).astype(F32).astype(BF16)


def swap_halves(v):
    return pltpu.roll(v, LANES // 2, 1)


def as_row(ref):
    wide = ref[...].astype(F32)
    return jnp.concatenate([wide[k : k + 1] for k in range(wide.shape[0])], axis=1)


def scale_pair(t, own, other):
    low = jnp.where(t == 0, own, other)
    high = jnp.where(t == 0, other, own)
    return jnp.where(lane_iota(low.shape) < LANES // 2, swap_halves(low), high)


def docs_kernel(own, docs, other, shares, out_ref, local_ref, edge_ref):
    t = lax.axis_index("tp")
    docs = landed(docs)[...]
    chip_rows = docs.shape[1]
    first = jnp.min(docs)
    last = jnp.max(docs)
    rows = chip_rows // 2
    hot = (docs == row_iota((DOCS, chip_rows))).astype(F32)
    hot_b = hot.astype(BF16)
    own_ref = landed(own)
    other_ref = landed(other)
    part = own_ref.shape[1]
    start = pl.multiple_of((1 - t) * rows, rows)
    tags = jnp.where(t == 0, docs[:, rows:], docs[:, :rows]) + 1
    edge_ref[:rows, :part] = own_ref[pl.ds(start, rows), :]
    edge_ref[:rows, part:] = other_ref[pl.ds(start, rows), :]
    edge_ref[rows:, :rows] = jnp.broadcast_to(tags.astype(F32), (16, rows)).astype(BF16)
    edge_ref[rows:, rows:] = jnp.zeros((16, 2 * part - rows), BF16)
    own_sums = dot(hot_b, own_ref[:, LANES : 2 * LANES])
    other_sums = dot(hot_b, other_ref[:, LANES : 2 * LANES])
    sums = scale_pair(t, own_sums, other_sums)
    counts = jnp.broadcast_to(jnp.sum(hot, axis=1, keepdims=True), (DOCS, LANES))
    here = row_iota((DOCS, LANES))
    local_ref[:, :LANES] = sums
    local_ref[:, LANES : 2 * LANES] = counts
    local_ref[:, 2 * LANES :] = ((here > first) & (here < last)).astype(F32)
    lane = lane_iota((1, LANES))

    def of(doc, values):
        return jnp.sum(jnp.where(here == doc, values, 0.0), axis=0, keepdims=True)

    meta = jnp.where(lane == 0, first.astype(F32), last.astype(F32))
    meta = jnp.where(lane == 2, of(first, counts), meta)
    meta = jnp.where(lane == 3, of(last, counts), meta)
    kind = row_iota(out_ref.shape) % 4
    out_ref[...] = jnp.where(
        kind == 0, of(first, sums), jnp.where(kind == 1, of(last, sums), meta)
    )
    out_ref[pl.ds(3, out_ref.shape[0] // 4, stride=4), :] = landed(shares)[...]


def slots_kernel(group, experts, share, slot_ref, shares_ref):
    slots, rows = slot_ref.shape
    groups = lax.axis_size("sp")
    ids = landed(group)[...]
    member = (ids == row_iota((groups, rows))).astype(F32)
    earlier = (row_iota((rows, rows)) < lane_iota((rows, rows))).astype(F32).astype(BF16)
    ranks = dot(member.astype(BF16), earlier) * member
    rank = jnp.sum(ranks, axis=0, keepdims=True).astype(jnp.int32)
    slot = ids * (slots // groups) + rank
    place = (row_iota((slots, rows)) == slot).astype(F32).astype(BF16)
    slot_ref[...] = place
    capacity = slots // groups
    spread = jnp.zeros((LANES, rows), F32)
    experts_ref, share_ref = landed(experts), landed(share)
    for k in range(experts_ref.shape[0]):
        chosen = experts_ref[k : k + 1, :] == row_iota((LANES, rows)) // capacity
        spread = spread + jnp.where(chosen, share_ref[k : k + 1, :].astype(F32), 0.0)
    each = dot(place, spread.astype(BF16), ((1,), (1,)))
    each = jnp.where(own_lane((slots, LANES), capacity), each, 0.0).astype(BF16)
    shares_ref[...] = dot(slot_source((groups, slots), capacity, 0), each)


def layout(rows):
    hot = rows
    local = hot + DOCS
    maps = local + DOCS
    gains = maps + LANES
    return hot, local, maps, gains


def windows_kernel(
    own,
    docs,
    other,
    edge,
    local_sums,
    weights,
    pool_gain,
    mixer_gain,
    routed_gain,
    bundle_ref,
    x_scr,
    tag_scr,
):
    t = lax.axis_index("tp")
    docs_ref = landed(docs)
    own_ref = landed(own)
    other_ref = landed(other)
    edge_ref = landed(edge)
    chip_rows, part = own_ref.shape
    rows = chip_rows // 2
    halo = rows
    span = chip_rows + halo
    tags = edge_ref[rows : rows + 1, :rows].astype(F32)

    @pl.when(t == 0)
    def _():
        x_scr[halo:, :part] = own_ref[...]
        x_scr[halo:, part:] = other_ref[...]
        x_scr[:halo, :] = edge_ref[:rows, :]
        tag_scr[:, halo:] = docs_ref[...].astype(F32) + 1.0
        tag_scr[:, :halo] = tags

    @pl.when(t == 1)
    def _():
        x_scr[:chip_rows, part:] = own_ref[...]
        x_scr[:chip_rows, :part] = other_ref[...]
        x_scr[chip_rows:, part:] = edge_ref[:rows, :part]
        x_scr[chip_rows:, :part] = edge_ref[:rows, part:]
        tag_scr[:, :chip_rows] = docs_ref[...].astype(F32) + 1.0
        tag_scr[:, chip_rows:] = tags

    hot = (tag_scr[...] == (row_iota((DOCS, span)) + 1).astype(F32)).astype(F32)
    center = hot[:, halo : halo + rows]
    hot_at, local_at, maps_at, gains_at = layout(rows)
    bundle_ref[hot_at:, :] = jnp.zeros((bundle_ref.shape[0] - hot_at, 2 * part), F32)
    bundle_ref[hot_at : hot_at + DOCS, :rows] = center
    same = dot(center.astype(BF16), hot.astype(BF16), ((0,), (0,))) > 0.5
    offset = lane_iota((rows, span)) - halo - row_iota((rows, span))
    x = x_scr[...]
    xc = x_scr[halo : halo + rows, :].astype(F32)
    level = (lane_iota((rows, 2 * part)) // 64) % 4
    diff = xc
    for k in range(3):
        half = chip_rows * (1 << k) // 8
        mask = (same & (offset >= -half) & (offset < half)).astype(F32)
        sums = dot(mask.astype(BF16), x)
        sizes = jnp.sum(mask, axis=1, keepdims=True)
        diff = jnp.where(level == k, sums / sizes - xc, diff)
    bundle_ref[:rows, :] = diff.astype(BF16).astype(F32)
    local_ref = landed(local_sums)
    bundle_ref[local_at : local_at + DOCS, : local_ref.shape[1]] = local_ref[...]
    weights_ref = landed(weights)
    dim = weights_ref.shape[1]
    spread = lane_iota((dim, LANES)) % dim == row_iota((dim, LANES))
    spread = spread.astype(F32).astype(BF16)
    keep = (row_iota((LANES, LANES)) // dim) == (lane_iota((LANES, LANES)) // dim)
    for k in range(4):
        pair = jnp.concatenate([weights_ref[2 * k], weights_ref[2 * k + 1]], axis=0)
        block = jnp.where(keep, dot(pair, spread), 0.0)
        bundle_ref[maps_at : maps_at + LANES, k * LANES : (k + 1) * LANES] = block
    at = gains_at
    for gain in (pool_gain, mixer_gain, routed_gain):
        row = as_row(landed(gain))
        for k in range(row.shape[1] // (2 * part)):
            bundle_ref[at : at + 1, :] = row[:, 2 * part * k : 2 * part * (k + 1)]
            at += 1


def inverse_rms(v):
    return lax.rsqrt(jnp.mean(v * v, axis=-1, keepdims=True) + EPSILON)


def mixer_kernel(
    bundle, output, residual, slot, info_ref, send_out, stream_out, send_ref, stream_ref, out_sems
):
    chips = info_ref.shape[0] // 4
    firsts, lasts, meta = (info_ref[pl.ds(k, chips, stride=4), :] for k in range(3))
    doc = lane_iota((chips, LANES)).astype(F32)
    first_id, last_id = meta[:, 0:1], meta[:, 1:2]
    is_first = (doc == first_id).astype(F32)
    is_last = ((doc == last_id) & (last_id != first_id)).astype(F32)
    wide = jnp.broadcast_to
    values = jnp.concatenate(
        [
            jnp.concatenate([firsts, wide(meta[:, 2:3], firsts.shape)], axis=1),
            jnp.concatenate([lasts, wide(meta[:, 3:4], lasts.shape)], axis=1),
        ],
        axis=0,
    )
    totals = dot(jnp.concatenate([is_first, is_last], axis=0), values, ((0,), (0,)), HIGHEST)
    bundle_ref = landed(bundle)
    rows = stream_ref.shape[0]
    width = stream_ref.shape[1]
    hot_at, local_at, maps_at, gains_at = layout(rows)
    local_ref = bundle_ref.at[local_at : local_at + DOCS]
    inside = local_ref[:, 2 * LANES : 3 * LANES] > 0.5
    sums = jnp.where(inside, local_ref[:, :LANES], totals[:DOCS, :LANES])
    counts = jnp.where(inside, local_ref[:, LANES : 2 * LANES], totals[:DOCS, LANES:])
    means = sums / jnp.maximum(counts, 1.0)
    hot = bundle_ref[hot_at : hot_at + DOCS, :rows]
    half = lane_iota((rows, LANES)) < LANES // 2
    x3 = jnp.where(
        half,
        swap_halves(bundle_ref[:rows, LANES : 2 * LANES]),
        bundle_ref[:rows, 3 * LANES : 4 * LANES],
    )
    diff3 = dot(hot, means, ((0,), (0,)), HIGHEST) - x3

    def gain_row(at, count):
        return jnp.concatenate([bundle_ref[at + k : at + k + 1, :] for k in range(count)], axis=1)

    span = bundle_ref.shape[1]
    parts = width // span
    gain = gain_row(gains_at, 1)
    pooled = []
    for k in range(4):
        cols = slice(k * LANES, (k + 1) * LANES)
        part = bundle_ref[:rows, cols]
        if k % 2 == 1:
            part = jnp.where(half, part, swap_halves(diff3) if k == 1 else diff3)
        channel_map = bundle_ref[maps_at : maps_at + LANES, cols].astype(BF16)
        pooled.append((dot(part.astype(BF16), channel_map) * gain[:, cols]).astype(BF16))
    mixed = dot(jnp.concatenate(pooled, axis=1), landed(output)[...])
    mixer_row = gain_row(gains_at + 1, parts)
    routed_row = gain_row(gains_at + 1 + parts, parts)
    stream = (
        landed(residual)[...].astype(F32) + mixed * inverse_rms(mixed) * mixer_row
    ).astype(BF16)
    stream_ref[...] = stream
    leaving = [pltpu.make_async_copy(stream_ref, stream_out, out_sems.at[0])]
    leaving[0].start()
    wide = stream.astype(F32)
    normed = (wide * inverse_rms(wide) * routed_row).astype(BF16)
    place = landed(slot)[...]
    for k in range(4):
        cols = slice(k * width // 4, (k + 1) * width // 4)
        send_ref[:, cols] = dot(place, normed[:, cols]).astype(BF16)
        leaving.append(
            pltpu.make_async_copy(send_ref.at[:, cols], send_out.at[:, cols], out_sems.at[k + 1])
        )
        leaving[-1].start()
    for copy in leaving:
        copy.wait()


def experts_kernel(
    rows_ref,
    info_ref,
    gate_ref,
    up_ref,
    down_ref,
    gate2_ref,
    up2_ref,
    down2_ref,
    out_ref,
    gates,
    ups,
    downs,
    acc,
    hidden,
    result,
    info,
    shares,
    sems,
    out_sems,
    first_sems,
):
    experts = gate_ref.shape[0]
    width = out_ref.shape[1]
    tile = 512
    units = gates.shape[2]
    steps = 2 * experts
    sources = [(gate_ref, up_ref, down_ref), (gate2_ref, up2_ref, down2_ref)]
    buffers = (gates, ups, downs)

    def copy(step, k):
        part, expert = step // experts, step % experts
        return pltpu.make_async_copy(
            sources[part][k].at[expert], buffers[k].at[step % 2], sems.at[k, step % 2]
        )

    def first(k, n):
        cols = slice(n * units // 2, (n + 1) * units // 2)
        return pltpu.make_async_copy(
            sources[0][k].at[0, :, cols], buffers[k].at[0, :, cols], first_sems.at[k, n]
        )

    def leave(cols, j):
        return pltpu.make_async_copy(result.at[:, cols], out_ref.at[:, cols], out_sems.at[j])

    def up_half(step, n):
        slot = step % 2
        cols = slice(n * units // 2, (n + 1) * units // 2)
        x = rows_ref[...]
        gate = dot(x, gates[slot, :, cols])
        upper = dot(x, ups[slot, :, cols])
        hidden[slot, :, cols] = (gate / (1.0 + jnp.exp(-gate)) * upper).astype(BF16)

    def down_tile(step, j):
        slot, expert = step % 2, step % experts
        cols = slice(j * tile, (j + 1) * tile)
        share = jnp.concatenate([shares[expert]] * (tile // LANES), axis=1)
        value = dot(hidden[slot], downs[slot, :, cols]) * share
        if expert > 0:
            value = acc[:, cols] + value
        if expert + 1 < experts:
            acc[:, cols] = value
        elif step < experts:
            result[:, cols] = value.astype(BF16)
        else:
            result[:, cols] = (
                result[:, cols].astype(F32) + value.astype(BF16).astype(F32)
            ).astype(BF16)
            leave(cols, j).start()

    tiles = width // tile
    told = pltpu.make_async_copy(info_ref, info, out_sems.at[0])
    told.start()
    for n in range(2):
        first(0, n).start()
        first(1, n).start()
    copy(0, 2).start()
    told.wait()
    slots = rows_ref.shape[0]
    groups = info.shape[0] // 4
    capacity = slots // groups
    sent = info[pl.ds(3, groups, stride=4), :].astype(BF16)
    sent = dot(slot_source((slots, groups), capacity, 1), sent)
    sent = jnp.where(own_lane((slots, LANES), capacity), sent, 0.0)
    for e in range(experts):
        one = jnp.where(lane_iota((slots, LANES)) // capacity == e, sent, 0.0)
        shares[e] = jnp.broadcast_to(jnp.sum(one, axis=1, keepdims=True), (slots, LANES))
    for step in range(steps + 1):
        if 0 < step < steps:
            copy(step, 0).wait()
            copy(step, 1).wait()
        if step > 0:
            copy(step - 1, 2).wait()
        if step + 1 < steps:
            copy(step + 1, 0).start()
            copy(step + 1, 1).start()
        for n in range(2):
            if step == 0:
                first(0, n).wait()
                first(1, n).wait()
            if step < steps:
                up_half(step, n)
            if step > 0:
                for j in range(n * tiles // 2, (n + 1) * tiles // 2):
                    down_tile(step - 1, j)
        if step + 1 < steps:
            copy(step + 1, 2).start()
    for j in range(tiles):
        leave(slice(j * tile, (j + 1) * tile), j).wait()


def final_kernel(gain_ref, back_ref, slot_ref, stream_ref, out_ref, held, sems):
    gain = as_row(gain_ref)
    count = sems.shape[0]
    step = held.shape[0] // count
    leaving = []
    for k in range(count):
        rows = slice(k * step, (k + 1) * step)
        value = dot(slot_ref[:, rows], back_ref[...], ((0,), (0,)))
        held[rows, :] = (
            stream_ref[rows, :].astype(F32) + value * inverse_rms(value) * gain
        ).astype(BF16)
        leaving.append(pltpu.make_async_copy(held.at[rows], out_ref.at[rows], sems.at[k]))
        leaving[-1].start()
    for copy in leaving:
        copy.wait()


def local(
    pool_input,
    documents,
    residual,
    group_weights,
    pool_gain,
    output_weight,
    mixer_gain,
    routed_gain,
    final_gain,
    chosen_group,
    chosen_experts,
    expert_share,
    expert_gate,
    expert_up,
    expert_down,
):
    chips = lax.axis_size("sp")
    chip_rows, part = pool_input.shape
    rows, width = residual.shape
    groups = chips
    capacity = chip_rows // groups
    slots = groups * capacity
    swap = [(0, 1), (1, 0)]
    both = ("sp", "tp")
    docs = documents.reshape(1, chip_rows)

    def tiles(gain):
        return gain.reshape(-1, LANES)

    other = lax.ppermute(pool_input, "tp", swap)
    gate2 = lax.ppermute(expert_gate, "tp", swap)
    up2 = lax.ppermute(expert_up, "tp", swap)
    down2 = lax.ppermute(expert_down, "tp", swap)
    slot, shares = call(
        slots_kernel,
        [((slots, rows), BF16), ((groups, LANES), F32)],
        (chosen_group.T, chosen_experts.T, expert_share.T),
        10**8,
    )
    info, local_sums, edge = call(
        docs_kernel,
        [
            ((chips * 4, LANES), F32),
            ((DOCS, 3 * LANES), F32),
            ((rows + 16, 2 * part), BF16),
        ],
        (pool_input, docs, other, shares),
        10**8,
    )
    same_core = [(2 * s, 2 * s + 2) for s in range(chips - 1)]
    same_core += [(2 * s + 1, 2 * s - 1) for s in range(1, chips)]
    edge = lax.ppermute(edge, both, same_core)
    info = lax.all_to_all(info.reshape(chips, 4, LANES), "sp", 0, 0, tiled=True)
    info = info.reshape(chips * 4, LANES)

    span = chip_rows + rows
    gain_rows = 1 + 2 * (width // (2 * part))
    (bundle,) = call(
        windows_kernel,
        [((layout(rows)[3] + 8 * pl.cdiv(gain_rows, 8), 2 * part), F32)],
        (
            pool_input,
            docs,
            other,
            edge,
            local_sums,
            group_weights,
            tiles(pool_gain),
            tiles(mixer_gain),
            tiles(routed_gain),
        ),
        10**9,
        scratch=[pltpu.VMEM((span, 2 * part), BF16), pltpu.VMEM((1, span), F32)],
    )
    send, stream = call(
        mixer_kernel,
        [((slots, width), BF16), ((rows, width), BF16)],
        (bundle, output_weight, residual, slot),
        2 * 10**9,
        near=(info,),
        spare=1640,
        outs=ANY,
        scratch=[
            pltpu.VMEM((slots, width), BF16),
            pltpu.VMEM((rows, width), BF16),
            pltpu.SemaphoreType.DMA((5,)),
        ],
    )
    arrived = lax.all_to_all(
        send.reshape(groups, capacity, width), "sp", 0, 0, tiled=True
    ).reshape(slots, width)
    units = expert_gate.shape[2]
    served = pl.pallas_call(
        experts_kernel,
        out_shape=jax.ShapeDtypeStruct((slots, width), BF16),
        in_specs=[VMEM] + [ANY] * 7,
        out_specs=ANY,
        scratch_shapes=[
            pltpu.VMEM((2, width, units), BF16),
            pltpu.VMEM((2, width, units), BF16),
            pltpu.VMEM((2, units, width), BF16),
            pltpu.VMEM((slots, width), F32),
            pltpu.VMEM((2, slots, units), BF16),
            pltpu.VMEM((slots, width), BF16),
            pltpu.VMEM((chips * 4, LANES), F32),
            pltpu.VMEM((expert_gate.shape[0], slots, LANES), F32),
            pltpu.SemaphoreType.DMA((3, 2)),
            pltpu.SemaphoreType.DMA((4,)),
            pltpu.SemaphoreType.DMA((2, 2)),
        ],
        cost_estimate=pl.CostEstimate(
            flops=2 * 10**10, bytes_accessed=40 * 10**6, transcendentals=0
        ),
        compiler_params=pltpu.CompilerParams(vmem_limit_bytes=48 * 1024 * 1024),
        name="experts",
    )(arrived, info, expert_gate, expert_up, expert_down, gate2, up2, down2)
    back = lax.all_to_all(
        served.reshape(groups, capacity, width), "sp", 0, 0, tiled=True
    ).reshape(slots, width)
    (out,) = call(
        final_kernel,
        [((rows, width), BF16)],
        (),
        10**9,
        near=(tiles(final_gain), back, slot, stream),
        spare=35 * 1024,
        outs=ANY,
        scratch=[pltpu.VMEM((rows, width), BF16), pltpu.SemaphoreType.DMA((2,))],
    )
    return out


def solution(mesh):
    placed = (
        P("sp", "tp"),
        P("sp"),
        P(("sp", "tp"), None),
        P(),
        P(),
        P(),
        P(),
        P(),
        P(),
        P(("sp", "tp"), None),
        P(("sp", "tp"), None),
        P(("sp", "tp"), None),
        P("sp", None, "tp"),
        P("sp", None, "tp"),
        P("sp", "tp", None),
    )

    return jax.shard_map(
        local, mesh=mesh, in_specs=placed, out_specs=P(("sp", "tp"), None), check_vma=False
    )
```
